32 devices in a mesh: sp: 4 (over y, x), tp: 8 (over z, core).
Axes of the slice: x: 2, y: 2, z: 4, core: 2. Of those that a mesh axis runs over, the one named last changes fastest.
Arguments:
- tokens: bfloat16 [2, 512, 4096], P(None, 'sp', 'tp'), may hold values from -6 to 6
- key_matrix: bfloat16 [4096, 4096], P(None, 'tp'), may hold values from -0.09375 to 0.09375
- value_matrix: bfloat16 [4096, 4096], P(None, 'tp'), may hold values from -0.375 to 0.375
- gate_matrix: bfloat16 [4096, 64], replicated, may hold values from -0.09375 to 0.09375
- head_decay_rate: float32 [32], P('tp'), may hold values from 0 to 1, as said below
- extra_log_decay: float32 [2, 32, 512], P(None, 'tp', 'sp'), may hold values from -3 to 0, as said below
- next_token_query: bfloat16 [2, 4096], P(None, 'tp'), may hold values from -6 to 6
- next_token_key: bfloat16 [2, 4096], P(None, 'tp'), may hold values from -6 to 6
- next_token_value: bfloat16 [2, 32, 128], P(None, 'tp', 'sp'), may hold values from -6 to 6
- next_write_strength: float32 [2, 32], P(None, 'tp'), may hold values from 0.05 to 1
- read_norm_gain: float32 [128], P('sp'), may hold values from 0.1 to 1.9
Outputs:
- state_cache: bfloat16 [2, 32, 128, 128], P(None, 'tp', None, 'sp')
- first_read: bfloat16 [2, 32, 128], P(None, 'tp', 'sp')
The draws below stay inside these ranges and needn't reach their ends.
Inputs may be any that keep to these rules, and one draw needn't show every extreme that they name: `head_decay_rate`: positive. `extra_log_decay`: never positive.
All inputs are finite; a program needn't handle non-finite values.
Results may differ from the reference program's by a relative error of at most 0.013.
Values may be sent and summed in bfloat16 or wider, within the bound.
No kernel may reach another device: no remote copies, remote signals or barrier semaphores. Data moves between devices by JAX's collectives and lax.ppermute only.
A program may use at most 64 MiB of HBM per device.

```python
import jax
import jax.numpy as jnp
from jax import lax

D = 4096
HEAD_COUNT = 32
DK = 128
DV = 128
PROMPT_COUNT = 2
POS_DEV = 128
BLOCK = 64
PROMPT_LENGTH = 512


def draw_head_decay_rate(key, part):
    chooser, fast_key, slow_key = jax.random.split(jax.random.fold_in(key, 11), 3)
    fast_share = 0.5
    fast_mask = jax.random.uniform(chooser, (HEAD_COUNT,), jnp.float32) < fast_share
    fast_rate = jnp.exp(jax.random.uniform(fast_key, (HEAD_COUNT,), jnp.float32, jnp.log(0.02), jnp.log(0.05)))
    slow_rate = jnp.exp(jax.random.uniform(slow_key, (HEAD_COUNT,), jnp.float32, jnp.log(0.05 / PROMPT_LENGTH), jnp.log(0.4 / PROMPT_LENGTH)))
    return jnp.where(fast_mask, fast_rate, slow_rate).astype(jnp.float32)


def draw_extra_log_decay(key, part):
    block_key, location_seed, magnitude_seed = jax.random.split(jax.random.fold_in(key, 23), 3)
    lowest_rate = 0.05
    highest_rate = 0.6
    block_total = PROMPT_LENGTH // POS_DEV
    block_rate = jnp.exp(jax.random.uniform(block_key, (PROMPT_COUNT, HEAD_COUNT, block_total), jnp.float32, jnp.log(lowest_rate / PROMPT_LENGTH), jnp.log(highest_rate / PROMPT_LENGTH)))
    position_decay = jnp.repeat(block_rate, POS_DEV, axis=2)
    spike_positions = jax.random.randint(location_seed, (PROMPT_COUNT, HEAD_COUNT, 2), 0, PROMPT_LENGTH)
    spike_magnitude = jnp.log(jax.random.uniform(magnitude_seed, (PROMPT_COUNT, HEAD_COUNT, 2), jnp.float32, 0.5, 0.8))
    spike_locations = jnp.arange(PROMPT_LENGTH, dtype=jnp.int32)
    decay_spikes = jnp.sum(jnp.where(spike_locations[None, None, None, :] == spike_positions[..., None], spike_magnitude[..., None], 0.0), axis=2)
    return (decay_spikes - position_decay).astype(jnp.float32)


def level_of(own_key, dims, shards, smallest, top_value):
    gain, own = 1.0, jax.random.fold_in(own_key, 6)
    for position, parts in shards:
        heights = jnp.exp(jax.random.uniform(jax.random.fold_in(own, position), (parts,), jnp.float32, smallest / len(shards), top_value / len(shards)))
        gain = gain * jnp.repeat(heights, dims[position] // parts).reshape([-1 if axis == position else 1 for axis in range(len(dims))])
    return gain


def bell_draw(own_key, shape, width, most, cuts=(), held_as=jnp.bfloat16):
    values = width * jax.random.normal(own_key, shape, jnp.float32)
    if cuts:
        values = values * level_of(own_key, shape, cuts, -0.22, 0.18)
    return jnp.clip(values, -most, most).astype(held_as)


def setup_inputs(seed: int = 0) -> dict:
    splits = jax.random.split(jax.random.key(seed), 12)
    return {
        "tokens": bell_draw(splits[0], (PROMPT_COUNT, PROMPT_LENGTH, D), 1.0, 6.0, ((1, 4), (2, 8))),
        "key_matrix": bell_draw(splits[1], (D, HEAD_COUNT * DK), D ** -0.5, 0.09375, ((1, 8),)),
        "value_matrix": bell_draw(splits[2], (D, HEAD_COUNT * DV), (D // 16) ** -0.5, 0.375, ((1, 8),)),
        "gate_matrix": bell_draw(splits[3], (D, 2 * HEAD_COUNT), D ** -0.5, 0.09375),
        "head_decay_rate": draw_head_decay_rate(jax.random.fold_in(splits[11], 71), 0),
        "extra_log_decay": draw_extra_log_decay(jax.random.fold_in(splits[11], 71), 0),
        "next_token_query": bell_draw(splits[6], (PROMPT_COUNT, HEAD_COUNT * DK), 1.0, 6.0, ((1, 8),)),
        "next_token_key": bell_draw(splits[7], (PROMPT_COUNT, HEAD_COUNT * DK), 1.0, 6.0, ((1, 8),)),
        "next_token_value": bell_draw(splits[8], (PROMPT_COUNT, HEAD_COUNT, DV), 1.0, 6.0, ((1, 8), (2, 4))),
        "next_write_strength": jnp.clip(0.05 + 0.95 * jax.random.uniform(splits[9], (PROMPT_COUNT, HEAD_COUNT), jnp.float32) ** level_of(splits[9], (PROMPT_COUNT, HEAD_COUNT), ((1, 8),), -0.2, 0.2), 0.05, 1.0),
        "read_norm_gain": jnp.clip(1.0 + 0.18 * jax.random.normal(splits[10], (DV,), jnp.float32), 0.1, 1.9),
    }


exact_mode = lax.Precision.HIGHEST
strength_offset = 5.0

def unit_rows(matrix):
    return matrix * lax.rsqrt(lax.optimization_barrier(jnp.sum(matrix * matrix, axis=-1, keepdims=True)) + 1e-06)

def nilpotent_inverse(mixing):
    extent = mixing.shape[-1]
    result = jnp.zeros_like(mixing) + jnp.eye(extent, dtype=jnp.float32)
    powered = -mixing
    covered = 1
    while covered < extent:
        result = result + jnp.einsum('...ij,...jk->...ik', result, powered, precision=exact_mode)
        powered = jnp.einsum('...ij,...jk->...ik', powered, powered, precision=exact_mode)
        covered = covered * 2
    return result

def block_terms(unit_keys, values, decay_logarithm, strength):
    extent = unit_keys.shape[-2]
    lower = jnp.tril(jnp.ones((extent, extent), jnp.bool_))
    strict = jnp.tril(jnp.ones((extent, extent), jnp.bool_), -1)
    running = jnp.cumsum(decay_logarithm, axis=-1)
    spread = running[..., :, None] - running[..., None, :]
    within = jnp.where(lower, jnp.exp(jnp.where(lower, spread, 0.0)), 0.0)
    scaled = unit_keys * strength[..., None]
    mixing = jnp.where(strict, jnp.einsum('...id,...jd->...ij', scaled, unit_keys, precision=exact_mode) * within, 0.0)
    inverse = nilpotent_inverse(mixing)
    writes = jnp.einsum('...ij,...je->...ie', inverse, values * strength[..., None], precision=exact_mode)
    erases = jnp.einsum('...ij,...jd->...id', inverse, scaled * jnp.exp(running)[..., None], precision=exact_mode)
    final_log = running[..., -1]
    carried = unit_keys * jnp.exp(final_log[..., None] - running)[..., None]
    return (writes, erases, carried, final_log)

def split_blocks(array, block_count):
    shaped = array.reshape(array.shape[:2] + (block_count, array.shape[2] // block_count) + array.shape[3:])
    return jnp.moveaxis(shaped, 2, 0)

def reference(tokens, key_matrix, value_matrix, gate_matrix, head_decay_rate, extra_log_decay, next_token_query, next_token_key, next_token_value, next_write_strength, read_norm_gain):
    key_proj = jnp.dot(tokens, key_matrix, preferred_element_type=jnp.float32).astype(jnp.bfloat16)
    value_proj = jnp.dot(tokens, value_matrix, preferred_element_type=jnp.float32).astype(jnp.bfloat16)
    gate_pre = jnp.dot(tokens, gate_matrix, preferred_element_type=jnp.float32)
    key_float = lax.optimization_barrier(key_proj).astype(jnp.float32)
    value_float = lax.optimization_barrier(value_proj).astype(jnp.float32)
    unit_keys = unit_rows(key_float.reshape(PROMPT_COUNT, PROMPT_LENGTH, HEAD_COUNT, DK).transpose(0, 2, 1, 3))
    values = value_float.reshape(PROMPT_COUNT, PROMPT_LENGTH, HEAD_COUNT, DV).transpose(0, 2, 1, 3)
    gate_projected = gate_pre.transpose(0, 2, 1)
    decay_logarithm = -head_decay_rate[None, :, None] * jax.nn.softplus(gate_projected[:, :HEAD_COUNT]) + extra_log_decay
    strength = jax.nn.sigmoid(gate_projected[:, HEAD_COUNT:] - strength_offset)
    block_count = PROMPT_LENGTH // BLOCK
    block_parts = block_terms(split_blocks(unit_keys, block_count), split_blocks(values, block_count), split_blocks(decay_logarithm, block_count), split_blocks(strength, block_count))

    def advance(current, block_part):
        writes, erases, carried, final_log = block_part
        fresh = writes - jnp.einsum('shcd,shde->shce', erases, current, precision=exact_mode)
        current = current * jnp.exp(final_log)[..., None, None] + jnp.einsum('shcd,shce->shde', carried, fresh, precision=exact_mode)
        return (current, None)
    start_state = jnp.zeros((PROMPT_COUNT, HEAD_COUNT, DK, DV), jnp.float32)
    state, _ = lax.scan(advance, start_state, block_parts)
    query_rows = next_token_query.astype(jnp.float32).reshape(PROMPT_COUNT, HEAD_COUNT, DK)
    unit_new = unit_rows(next_token_key.astype(jnp.float32).reshape(PROMPT_COUNT, HEAD_COUNT, DK))
    value_rows = next_token_value.astype(jnp.float32)
    key_read = jnp.einsum('shd,shde->she', unit_new, state, precision=exact_mode)
    query_read = jnp.einsum('shd,shde->she', query_rows, state, precision=exact_mode)
    intersection = lax.optimization_barrier(jnp.sum(query_rows * unit_new, axis=-1))
    read_raw = query_read + (next_write_strength * intersection)[..., None] * (value_rows - key_read)
    first_read = read_raw * lax.rsqrt(lax.optimization_barrier(jnp.mean(read_raw * read_raw, axis=-1, keepdims=True)) + 1e-06) * read_norm_gain
    return (state.astype(jnp.bfloat16), first_read.astype(jnp.bfloat16))
```

```python
import functools

import jax
import jax.numpy as jnp
from jax import lax
from jax.experimental import pallas as pl
from jax.experimental.pallas import tpu as pltpu
from jax.sharding import PartitionSpec as P

DV = 128


exact_mode = lax.Precision.HIGHEST
strength_offset = 5.0


def unit_rows(matrix):
    return matrix * lax.rsqrt(jnp.sum(matrix * matrix, axis=-1, keepdims=True) + 1e-06)


def nilpotent_inverse(mixing):
    extent = mixing.shape[-1]
    result = jnp.zeros_like(mixing) + jnp.eye(extent, dtype=jnp.float32)
    powered = -mixing
    covered = 1
    while covered < extent:
        product = lax.optimization_barrier(
            jnp.einsum("...ij,...jk->...ik", result, powered, precision=exact_mode)
        )
        result = result + product
        powered = jnp.einsum("...ij,...jk->...ik", powered, powered, precision=exact_mode)
        covered = covered * 2
    return result


def block_terms(unit_keys, values, decay_logarithm, strength):
    extent = unit_keys.shape[-2]
    lower = jnp.tril(jnp.ones((extent, extent), jnp.bool_))
    strict = jnp.tril(jnp.ones((extent, extent), jnp.bool_), -1)
    running = jnp.cumsum(decay_logarithm, axis=-1)
    spread = running[..., :, None] - running[..., None, :]
    within = jnp.where(lower, jnp.exp(jnp.where(lower, spread, 0.0)), 0.0)
    scaled = unit_keys * strength[..., None]
    mixing = jnp.where(
        strict,
        jnp.einsum("...id,...jd->...ij", scaled, unit_keys, precision=exact_mode) * within,
        0.0,
    )
    inverse = nilpotent_inverse(mixing)
    writes = jnp.einsum(
        "...ij,...je->...ie", inverse, values * strength[..., None], precision=exact_mode
    )
    erases = jnp.einsum(
        "...ij,...jd->...id", inverse, scaled * jnp.exp(running)[..., None], precision=exact_mode
    )
    final_log = running[..., -1]
    carried = unit_keys * jnp.exp(final_log[..., None] - running)[..., None]
    return (writes, erases, carried, final_log)


def split_blocks(array, block_count):
    shaped = array.reshape(
        array.shape[:2] + (block_count, array.shape[2] // block_count) + array.shape[3:]
    )
    return jnp.moveaxis(shaped, 2, 0)


def local(
    tokens,
    key_matrix,
    value_matrix,
    gate_matrix,
    head_decay_rate,
    extra_log_decay,
    next_token_query,
    next_token_key,
    next_token_value,
    next_write_strength,
    read_norm_gain,
):
    sequences, positions, _ = tokens.shape
    local_heads = head_decay_rate.shape[0]
    key_width = key_matrix.shape[1] // local_heads
    value_width = value_matrix.shape[1] // local_heads
    all_heads = gate_matrix.shape[1] // 2
    group_size = lax.axis_size("sp")
    column_share = value_width // group_size
    first_head = lax.axis_index("tp") * local_heads
    decay_cols = lax.dynamic_slice_in_dim(gate_matrix, first_head, local_heads, 1)
    strength_cols = lax.dynamic_slice_in_dim(gate_matrix, all_heads + first_head, local_heads, 1)
    gate_cols = jnp.concatenate([decay_cols, strength_cols], axis=1)
    row_count = sequences * positions
    incoming = lax.all_gather(tokens, "tp", axis=2, tiled=True)
    span_width = incoming.shape[2]
    flat_rows = incoming.reshape(row_count, span_width)
    products = lax.optimization_barrier(
        (
            jnp.dot(flat_rows, key_matrix, preferred_element_type=jnp.float32),
            jnp.dot(flat_rows, value_matrix, preferred_element_type=jnp.float32),
            jnp.dot(flat_rows, gate_cols, preferred_element_type=jnp.float32),
        )
    )
    key_sum = products[0]
    value_sum = products[1]
    gate_pre = products[2]
    key_float = lax.optimization_barrier(key_sum.astype(jnp.bfloat16)).astype(jnp.float32)
    value_float = lax.optimization_barrier(value_sum.astype(jnp.bfloat16)).astype(jnp.float32)
    unit_keys = unit_rows(
        key_float.reshape(sequences, positions, local_heads, key_width).transpose(0, 2, 1, 3)
    )
    values = value_float.reshape(sequences, positions, local_heads, value_width).transpose(
        0, 2, 1, 3
    )
    gate_projected = gate_pre.reshape(sequences, positions, 2 * local_heads).transpose(0, 2, 1)
    decay_logarithm = (
        -head_decay_rate[None, :, None] * jax.nn.softplus(gate_projected[:, :local_heads])
        + extra_log_decay
    )
    strength = jax.nn.sigmoid(gate_projected[:, local_heads:] - strength_offset)
    block_count = positions // min(64, positions)
    block_parts = block_terms(
        split_blocks(unit_keys, block_count),
        split_blocks(values, block_count),
        split_blocks(decay_logarithm, block_count),
        split_blocks(strength, block_count),
    )
    identity = jnp.zeros((sequences, local_heads, key_width, key_width), jnp.float32) + jnp.eye(
        key_width, dtype=jnp.float32
    )
    start_map = jnp.concatenate(
        [identity, jnp.zeros((sequences, local_heads, key_width, value_width), jnp.float32)],
        axis=-1,
    )

    def advance(current, block_part):
        writes, erases, carried, final_log = block_part
        padded = jnp.concatenate(
            [jnp.zeros(writes.shape[:-1] + (key_width,), jnp.float32), writes], axis=-1
        )
        removed = lax.optimization_barrier(
            jnp.einsum("shcd,shde->shce", erases, current, precision=exact_mode)
        )
        fresh = padded - removed
        added = lax.optimization_barrier(
            jnp.einsum("shcd,shce->shde", carried, fresh, precision=exact_mode)
        )
        current = current * jnp.exp(final_log)[..., None, None] + added
        return (current, None)

    local_map, _ = lax.scan(advance, start_map, block_parts)
    carry_map = local_map[..., :key_width]
    write_map = local_map[..., key_width:]
    carry_copies = jnp.broadcast_to(carry_map[None], (group_size,) + carry_map.shape)
    write_parts = jnp.moveaxis(
        write_map.reshape(sequences, local_heads, key_width, group_size, column_share), 3, 0
    )
    carries = lax.all_to_all(carry_copies, "sp", split_axis=0, concat_axis=0, tiled=True)
    write_cols = lax.all_to_all(write_parts, "sp", split_axis=0, concat_axis=0, tiled=True)

    def fold_step(current, block_map):
        moved = lax.optimization_barrier(
            jnp.einsum("shij,shje->shie", block_map[0], current, precision=exact_mode)
        )
        return (moved + block_map[1], None)

    begin_state = jnp.zeros(write_cols.shape[1:], jnp.float32)
    folded, _ = lax.scan(fold_step, begin_state, (carries, write_cols))
    query_rows = next_token_query.astype(jnp.float32).reshape(sequences, local_heads, key_width)
    unit_new = unit_rows(
        next_token_key.astype(jnp.float32).reshape(sequences, local_heads, key_width)
    )
    value_rows = next_token_value.astype(jnp.float32)
    key_read = jnp.einsum("shd,shde->she", unit_new, folded, precision=exact_mode)
    query_read = jnp.einsum("shd,shde->she", query_rows, folded, precision=exact_mode)
    intersection = jnp.sum(query_rows * unit_new, axis=-1)
    read_raw = query_read + (next_write_strength * intersection)[..., None] * (
        value_rows - key_read
    )
    square_total = lax.psum(jnp.sum(read_raw * read_raw, axis=-1, keepdims=True), "sp")
    first_read = read_raw * lax.rsqrt(square_total / DV + 1e-06) * read_norm_gain
    return (folded.astype(jnp.bfloat16), first_read.astype(jnp.bfloat16))

def split3(value):
    first = value.astype(jnp.bfloat16).astype(jnp.float32)
    rest = value - first
    second = rest.astype(jnp.bfloat16).astype(jnp.float32)
    return first, second, rest - second


def dot_nn(left, right, precision=None):
    return lax.dot_general(
        left, right, (((1,), (0,)), ((), ())), precision=precision, preferred_element_type=jnp.float32
    )


def dot_nt(left, right, precision=None):
    return lax.dot_general(
        left, right, (((1,), (1,)), ((), ())), precision=precision, preferred_element_type=jnp.float32
    )


def dot_tn(left, right, precision=None):
    return lax.dot_general(
        left, right, (((0,), (0,)), ((), ())), precision=precision, preferred_element_type=jnp.float32
    )


SIDE = 16


def project_kernel(sources, group, *refs):
    count = len(sources)
    pieces = refs[:count]
    key_ref, value_ref, gate_ref, rate_ref, extra_ref, fresh_ref, gain_ref = refs[count : count + 7]
    outs = refs[count + 7 : count + 7 + group]
    key_sum, value_sum, decay_rows, strength_rows = refs[count + 7 + group :]
    me = lax.axis_index("tp")
    place = lax.axis_index("sp")
    sequences, heads, positions = extra_ref.shape
    depth = pieces[0].shape[1]
    width = key_ref.shape[1] // heads
    share = heads // group
    total_key = total_value = total_gate = None
    for piece, (lane, step) in zip(pieces, sources):
        owner = (((me // 2) ^ step) * 2) + ((me % 2) ^ lane)
        rows = pl.ds(pl.multiple_of(owner * depth, depth), depth)
        block = piece[...]
        part_key = dot_nn(block, key_ref[rows, :])
        part_value = dot_nn(block, value_ref[rows, :])
        part_gate = dot_nt(gate_ref[:, rows], block)
        total_key = part_key if total_key is None else total_key + part_key
        total_value = part_value if total_value is None else total_value + part_value
        total_gate = part_gate if total_gate is None else total_gate + part_gate
    key_sum[...] = total_key.astype(jnp.bfloat16)
    value_sum[...] = total_value.astype(jnp.bfloat16)
    row_at = lax.broadcasted_iota(jnp.int32, (positions, positions), 0)
    col_at = lax.broadcasted_iota(jnp.int32, (positions, positions), 1)
    upper = (row_at <= col_at).astype(jnp.float32)
    for s in range(sequences):
        gates = total_gate[:, s * positions : (s + 1) * positions]
        decay = -rate_ref[...] * jax.nn.softplus(gates[:heads]) + extra_ref[s]
        decay_rows[s] = dot_nn(decay, upper, exact_mode)
        strength_rows[s] = jax.nn.sigmoid(gates[heads : 2 * heads] - strength_offset)
    gain_parts = split3(gain_ref[...])
    for m in range(group):
        peer = place ^ m
        for s in range(sequences):
            for r in range(share):
                head = peer * share + r
                columns = pl.ds(pl.multiple_of(head * width, width), width)
                span = pl.ds(s * positions, positions)
                outs[m][s, r, pl.ds(0, positions), :] = key_sum[span, columns]
                outs[m][s, r, pl.ds(positions, positions), :] = value_sum[span, columns]
                side = [
                    *split3(decay_rows[s, pl.ds(head, 1), :]),
                    *split3(strength_rows[s, pl.ds(head, 1), :]),
                    fresh_ref[s, pl.ds(head, 1), :],
                    *gain_parts,
                ]
                side.append(jnp.zeros((SIDE - len(side), positions), jnp.float32))
                outs[m][s, r, pl.ds(2 * positions, SIDE), :] = jnp.concatenate(side, axis=0).astype(
                    jnp.bfloat16
                )


def unit_lower_inverse(mixing, row_at, col_at):
    extent = mixing.shape[0]
    small = 16
    eye = (row_at == col_at).astype(jnp.float32)
    powered = jnp.where(row_at // small == col_at // small, -mixing, 0.0)
    result = eye + powered
    covered = 2
    while covered < small:
        powered = dot_nn(powered, powered, exact_mode)
        result = result + dot_nn(result, powered, exact_mode)
        covered *= 2
    size = small
    while size < extent:
        joins = (row_at // (2 * size) == col_at // (2 * size)) & (row_at // size > col_at // size)
        corner = jnp.where(joins, mixing, 0.0)
        result = result - dot_nn(dot_nn(result, corner, exact_mode), result, exact_mode)
        size *= 2
    return result


def state_kernel(group, *refs):
    blocks = refs[:group]
    query_ref, new_key_ref, new_strength_ref = refs[group : group + 3]
    outs = refs[group + 3 : 2 * group + 3]
    maps, adds, turned = refs[2 * group + 3 :]
    place = lax.axis_index("sp")
    sequences, share = blocks[0].shape[:2]
    positions = (blocks[0].shape[2] - SIDE) // 2
    width = blocks[0].shape[3]
    row_at = lax.broadcasted_iota(jnp.int32, (positions, positions), 0)
    col_at = lax.broadcasted_iota(jnp.int32, (positions, positions), 1)
    for s in range(sequences):
        for r in range(share):
            fresh_row = gain_row = None
            for m in range(group):
                keys = blocks[m][s, r, pl.ds(0, positions), :]
                values = blocks[m][s, r, pl.ds(positions, positions), :]
                side = blocks[m][s, r, pl.ds(2 * positions, SIDE), :].astype(jnp.float32)
                decay_row = side[0:1] + side[1:2] + side[2:3]
                strength_row = side[3:4] + side[4:5] + side[5:6]
                fresh_row = side[6:7] if fresh_row is None else fresh_row + side[6:7]
                gain = side[7:8] + side[8:9] + side[9:10]
                gain_row = gain if gain_row is None else gain_row + gain
                stacked = jnp.concatenate(
                    [decay_row, strength_row, jnp.zeros((6, positions), jnp.float32)], axis=0
                ).T
                decay_col = stacked[:, 0:1]
                strength_col = stacked[:, 1:2]
                wide = keys.astype(jnp.float32)
                scale_col = lax.rsqrt(jnp.sum(wide * wide, axis=-1, keepdims=True) + 1e-06)
                unit = wide * scale_col
                spread = decay_col - decay_row
                within = jnp.exp(jnp.where(row_at >= col_at, spread, 0.0))
                mixing = jnp.where(
                    row_at > col_at,
                    dot_nt(unit * strength_col, unit, exact_mode) * within,
                    0.0,
                )
                inverse = unit_lower_inverse(mixing, row_at, col_at)
                final_log = decay_row[:, positions - 1 :]
                scaled = unit * (strength_col * jnp.exp(decay_col))
                writes = dot_nn(inverse, values.astype(jnp.float32) * strength_col, exact_mode)
                erases = dot_nn(inverse, scaled, exact_mode)
                carried = unit * jnp.exp(final_log - decay_col)
                place_of = (place ^ m)
                maps[place_of] = jnp.where(row_at == col_at, jnp.exp(final_log), 0.0) - dot_tn(
                    erases, carried, exact_mode
                )
                adds[place_of] = dot_tn(writes, carried, exact_mode)
            state = adds[0]
            for b in range(1, group):
                state = dot_nn(state, maps[b], exact_mode) + adds[b]
            head = place * share + r
            query = query_ref[s, pl.ds(head, 1), :].astype(jnp.float32)
            new_key = new_key_ref[s, pl.ds(head, 1), :].astype(jnp.float32)
            unit_new = new_key * lax.rsqrt(jnp.sum(new_key * new_key, axis=-1, keepdims=True) + 1e-06)
            both = jnp.concatenate([query, unit_new, jnp.zeros((6, width), jnp.float32)], axis=0)
            reads = dot_nt(both, state, exact_mode)
            overlap = jnp.sum(query * unit_new, axis=-1, keepdims=True)
            raw = reads[0:1] + new_strength_ref[s, pl.ds(head, 1), :] * overlap * (
                fresh_row - reads[1:2]
            )
            first = raw * lax.rsqrt(jnp.mean(raw * raw, axis=-1, keepdims=True) + 1e-06) * gain_row
            turned[...] = state.astype(jnp.bfloat16)
            tail = jnp.broadcast_to(first, (SIDE, positions)).astype(jnp.bfloat16)
            column_share = turned.shape[0] // group
            for m in range(group):
                rows = pl.ds(pl.multiple_of((place ^ m) * column_share, column_share), column_share)
                outs[m][s, r, pl.ds(0, column_share), :] = turned[rows, :]
                outs[m][s, r, pl.ds(column_share, SIDE), :] = tail


def finish_kernel(group, *refs):
    parts = refs[:group]
    state_ref, read_ref, reads = refs[group:]
    place = lax.axis_index("sp")
    sequences, share, rows, width = parts[0].shape
    column_share = rows - SIDE
    for m in range(group):
        for s in range(sequences):
            for r in range(share):
                head = (place ^ m) * share + r
                state_ref[s, head] = parts[m][s, r, pl.ds(0, column_share), :]
                line = pltpu.roll(
                    parts[m][s, r, pl.ds(column_share, SIDE), :].astype(jnp.float32)[:8],
                    (group - place) * column_share,
                    1,
                )
                reads[s, pl.ds(head, 1), :] = line[0:1, :column_share]
    read_ref[...] = reads[...].astype(jnp.bfloat16)


def fast_local(
    tokens,
    key_matrix,
    value_matrix,
    gate_matrix,
    head_decay_rate,
    extra_log_decay,
    next_token_query,
    next_token_key,
    next_token_value,
    next_write_strength,
    read_norm_gain,
):
    sequences, positions, depth = tokens.shape
    heads = head_decay_rate.shape[0]
    all_heads = gate_matrix.shape[1] // 2
    group = lax.axis_size("sp")
    members = lax.axis_size("tp")
    share = heads // group
    width = key_matrix.shape[1] // heads
    column_share = next_token_value.shape[2]
    value_width = column_share * group
    place = lax.axis_index("sp")
    first_head = lax.axis_index("tp") * heads
    f32, bf16 = jnp.float32, jnp.bfloat16
    gate_rows = jnp.concatenate(
        [
            lax.dynamic_slice_in_dim(gate_matrix, first_head, heads, 1),
            lax.dynamic_slice_in_dim(gate_matrix, all_heads + first_head, heads, 1),
        ],
        axis=1,
    ).T
    rate_rows = jnp.broadcast_to(head_decay_rate[:, None], (heads, positions))
    fresh_rows = lax.dynamic_update_slice_in_dim(
        jnp.zeros((sequences, heads, value_width), f32),
        next_token_value.astype(f32),
        place * column_share,
        2,
    )
    gain_row = lax.dynamic_update_slice_in_dim(
        jnp.zeros((1, value_width), f32), read_norm_gain[None], place * column_share, 1
    )
    query = next_token_query.reshape(sequences, heads, width).astype(f32)
    new_key = next_token_key.reshape(sequences, heads, width).astype(f32)
    new_strength = jnp.broadcast_to(next_write_strength[..., None], (sequences, heads, width))

    def over_tp(array, step):
        pairs = [((z * 2 + c), (z ^ step) * 2 + c) for z in range(members // 2) for c in range(2)]
        return lax.ppermute(array, "tp", pairs)

    def to_partner(array):
        return lax.ppermute(array, "tp", [(i, i ^ 1) for i in range(members)])

    def over_sp(array, step):
        return lax.ppermute(array, "sp", [(i, i ^ step) for i in range(group)])

    own = tokens.reshape(sequences * positions, depth)
    sources, pieces = [(0, 0), (1, 0)], [own, to_partner(own)]
    for step in range(members // 2 - 1, 0, -1):
        got = over_tp(own, step)
        sources += [(0, step), (1, step)]
        pieces += [got, to_partner(got)]
    rows = 2 * positions + SIDE
    vmem = pl.BlockSpec(memory_space=pltpu.VMEM)
    messages = pl.pallas_call(
        functools.partial(project_kernel, sources, group),
        out_shape=[jax.ShapeDtypeStruct((sequences, share, rows, width), bf16)] * group,
        in_specs=[vmem] * (len(pieces) + 7),
        out_specs=[vmem] * group,
        scratch_shapes=[
            pltpu.VMEM((sequences * positions, key_matrix.shape[1]), bf16),
            pltpu.VMEM((sequences * positions, value_matrix.shape[1]), bf16),
            pltpu.VMEM((sequences, heads, positions), f32),
            pltpu.VMEM((sequences, heads, positions), f32),
        ],
        compiler_params=pltpu.CompilerParams(vmem_limit_bytes=24 * 2**20),
        name="project",
    )(
        *pieces,
        key_matrix,
        value_matrix,
        gate_rows,
        rate_rows,
        extra_log_decay,
        fresh_rows,
        gain_row,
    )
    blocks = [messages[0]] + [over_sp(messages[m], m) for m in range(1, group)]
    out_rows = column_share + SIDE
    results = pl.pallas_call(
        functools.partial(state_kernel, group),
        out_shape=[jax.ShapeDtypeStruct((sequences, share, out_rows, width), bf16)] * group,
        in_specs=[vmem] * (group + 3),
        out_specs=[vmem] * group,
        scratch_shapes=[
            pltpu.VMEM((group, value_width, width), f32),
            pltpu.VMEM((group, value_width, width), f32),
            pltpu.VMEM((value_width, width), bf16),
        ],
        compiler_params=pltpu.CompilerParams(vmem_limit_bytes=8 * 2**20),
        name="state",
    )(*blocks, query, new_key, new_strength)
    parts = [results[0]] + [over_sp(results[m], m) for m in range(1, group)]
    turned_state, first_read = pl.pallas_call(
        functools.partial(finish_kernel, group),
        out_shape=[
            jax.ShapeDtypeStruct((sequences, heads, column_share, width), bf16),
            jax.ShapeDtypeStruct((sequences, heads, column_share), bf16),
        ],
        in_specs=[vmem] * group,
        out_specs=[vmem] * 2,
        scratch_shapes=[pltpu.VMEM((sequences, heads, column_share), f32)],
        compiler_params=pltpu.CompilerParams(vmem_limit_bytes=4 * 2**20),
        name="finish",
    )(*parts)
    return turned_state.transpose(0, 1, 3, 2), first_read


def pick(mesh):
    def body(*args):
        group, members = mesh.shape["sp"], mesh.shape["tp"]
        tokens, heads = args[0], args[4].shape[0]
        powers = group & (group - 1) == 0 and members & (members - 1) == 0
        square = args[1].shape[1] // heads == tokens.shape[1] == args[2].shape[1] // heads
        if powers and members > 1 and heads % group == 0 and square:
            return fast_local(*args)
        return local(*args)

    return body


def solution(mesh):
    in_specs = (
        P(None, "sp", "tp"),
        P(None, "tp"),
        P(None, "tp"),
        P(),
        P("tp"),
        P(None, "tp", "sp"),
        P(None, "tp"),
        P(None, "tp"),
        P(None, "tp", "sp"),
        P(None, "tp"),
        P("sp"),
    )
    out_specs = (P(None, "tp", None, "sp"), P(None, "tp", "sp"))
    return jax.shard_map(
        pick(mesh), mesh=mesh, in_specs=in_specs, out_specs=out_specs, check_vma=False)
```

```python
import functools

import jax
import jax.numpy as jnp
from jax import lax
from jax.experimental import pallas as pl
from jax.experimental.pallas import tpu as pltpu
from jax.sharding import PartitionSpec as P

DV = 128


exact_mode = lax.Precision.HIGHEST
strength_offset = 5.0


def unit_rows(matrix):
    return matrix * lax.rsqrt(jnp.sum(matrix * matrix, axis=-1, keepdims=True) + 1e-06)


def nilpotent_inverse(mixing):
    extent = mixing.shape[-1]
    result = jnp.zeros_like(mixing) + jnp.eye(extent, dtype=jnp.float32)
    powered = -mixing
    covered = 1
    while covered < extent:
        product = lax.optimization_barrier(
            jnp.einsum("...ij,...jk->...ik", result, powered, precision=exact_mode)
        )
        result = result + product
        powered = jnp.einsum("...ij,...jk->...ik", powered, powered, precision=exact_mode)
        covered = covered * 2
    return result


def block_terms(unit_keys, values, decay_logarithm, strength):
    extent = unit_keys.shape[-2]
    lower = jnp.tril(jnp.ones((extent, extent), jnp.bool_))
    strict = jnp.tril(jnp.ones((extent, extent), jnp.bool_), -1)
    running = jnp.cumsum(decay_logarithm, axis=-1)
    spread = running[..., :, None] - running[..., None, :]
    within = jnp.where(lower, jnp.exp(jnp.where(lower, spread, 0.0)), 0.0)
    scaled = unit_keys * strength[..., None]
    mixing = jnp.where(
        strict,
        jnp.einsum("...id,...jd->...ij", scaled, unit_keys, precision=exact_mode) * within,
        0.0,
    )
    inverse = nilpotent_inverse(mixing)
    writes = jnp.einsum(
        "...ij,...je->...ie", inverse, values * strength[..., None], precision=exact_mode
    )
    erases = jnp.einsum(
        "...ij,...jd->...id", inverse, scaled * jnp.exp(running)[..., None], precision=exact_mode
    )
    final_log = running[..., -1]
    carried = unit_keys * jnp.exp(final_log[..., None] - running)[..., None]
    return (writes, erases, carried, final_log)


def split_blocks(array, block_count):
    shaped = array.reshape(
        array.shape[:2] + (block_count, array.shape[2] // block_count) + array.shape[3:]
    )
    return jnp.moveaxis(shaped, 2, 0)


def local(
    tokens,
    key_matrix,
    value_matrix,
    gate_matrix,
    head_decay_rate,
    extra_log_decay,
    next_token_query,
    next_token_key,
    next_token_value,
    next_write_strength,
    read_norm_gain,
):
    sequences, positions, _ = tokens.shape
    local_heads = head_decay_rate.shape[0]
    key_width = key_matrix.shape[1] // local_heads
    value_width = value_matrix.shape[1] // local_heads
    all_heads = gate_matrix.shape[1] // 2
    group_size = lax.axis_size("sp")
    column_share = value_width // group_size
    first_head = lax.axis_index("tp") * local_heads
    decay_cols = lax.dynamic_slice_in_dim(gate_matrix, first_head, local_heads, 1)
    strength_cols = lax.dynamic_slice_in_dim(gate_matrix, all_heads + first_head, local_heads, 1)
    gate_cols = jnp.concatenate([decay_cols, strength_cols], axis=1)
    row_count = sequences * positions
    incoming = lax.all_gather(tokens, "tp", axis=2, tiled=True)
    span_width = incoming.shape[2]
    flat_rows = incoming.reshape(row_count, span_width)
    products = lax.optimization_barrier(
        (
            jnp.dot(flat_rows, key_matrix, preferred_element_type=jnp.float32),
            jnp.dot(flat_rows, value_matrix, preferred_element_type=jnp.float32),
            jnp.dot(flat_rows, gate_cols, preferred_element_type=jnp.float32),
        )
    )
    key_sum = products[0]
    value_sum = products[1]
    gate_pre = products[2]
    key_float = lax.optimization_barrier(key_sum.astype(jnp.bfloat16)).astype(jnp.float32)
    value_float = lax.optimization_barrier(value_sum.astype(jnp.bfloat16)).astype(jnp.float32)
    unit_keys = unit_rows(
        key_float.reshape(sequences, positions, local_heads, key_width).transpose(0, 2, 1, 3)
    )
    values = value_float.reshape(sequences, positions, local_heads, value_width).transpose(
        0, 2, 1, 3
    )
    gate_projected = gate_pre.reshape(sequences, positions, 2 * local_heads).transpose(0, 2, 1)
    decay_logarithm = (
        -head_decay_rate[None, :, None] * jax.nn.softplus(gate_projected[:, :local_heads])
        + extra_log_decay
    )
    strength = jax.nn.sigmoid(gate_projected[:, local_heads:] - strength_offset)
    block_count = positions // min(64, positions)
    block_parts = block_terms(
        split_blocks(unit_keys, block_count),
        split_blocks(values, block_count),
        split_blocks(decay_logarithm, block_count),
        split_blocks(strength, block_count),
    )
    identity = jnp.zeros((sequences, local_heads, key_width, key_width), jnp.float32) + jnp.eye(
        key_width, dtype=jnp.float32
    )
    start_map = jnp.concatenate(
        [identity, jnp.zeros((sequences, local_heads, key_width, value_width), jnp.float32)],
        axis=-1,
    )

    def advance(current, block_part):
        writes, erases, carried, final_log = block_part
        padded = jnp.concatenate(
            [jnp.zeros(writes.shape[:-1] + (key_width,), jnp.float32), writes], axis=-1
        )
        removed = lax.optimization_barrier(
            jnp.einsum("shcd,shde->shce", erases, current, precision=exact_mode)
        )
        fresh = padded - removed
        added = lax.optimization_barrier(
            jnp.einsum("shcd,shce->shde", carried, fresh, precision=exact_mode)
        )
        current = current * jnp.exp(final_log)[..., None, None] + added
        return (current, None)

    local_map, _ = lax.scan(advance, start_map, block_parts)
    carry_map = local_map[..., :key_width]
    write_map = local_map[..., key_width:]
    carry_copies = jnp.broadcast_to(carry_map[None], (group_size,) + carry_map.shape)
    write_parts = jnp.moveaxis(
        write_map.reshape(sequences, local_heads, key_width, group_size, column_share), 3, 0
    )
    carries = lax.all_to_all(carry_copies, "sp", split_axis=0, concat_axis=0, tiled=True)
    write_cols = lax.all_to_all(write_parts, "sp", split_axis=0, concat_axis=0, tiled=True)

    def fold_step(current, block_map):
        moved = lax.optimization_barrier(
            jnp.einsum("shij,shje->shie", block_map[0], current, precision=exact_mode)
        )
        return (moved + block_map[1], None)

    begin_state = jnp.zeros(write_cols.shape[1:], jnp.float32)
    folded, _ = lax.scan(fold_step, begin_state, (carries, write_cols))
    query_rows = next_token_query.astype(jnp.float32).reshape(sequences, local_heads, key_width)
    unit_new = unit_rows(
        next_token_key.astype(jnp.float32).reshape(sequences, local_heads, key_width)
    )
    value_rows = next_token_value.astype(jnp.float32)
    key_read = jnp.einsum("shd,shde->she", unit_new, folded, precision=exact_mode)
    query_read = jnp.einsum("shd,shde->she", query_rows, folded, precision=exact_mode)
    intersection = jnp.sum(query_rows * unit_new, axis=-1)
    read_raw = query_read + (next_write_strength * intersection)[..., None] * (
        value_rows - key_read
    )
    square_total = lax.psum(jnp.sum(read_raw * read_raw, axis=-1, keepdims=True), "sp")
    first_read = read_raw * lax.rsqrt(square_total / DV + 1e-06) * read_norm_gain
    return (folded.astype(jnp.bfloat16), first_read.astype(jnp.bfloat16))


def split3(value):
    first = value.astype(jnp.bfloat16).astype(jnp.float32)
    rest = value - first
    second = rest.astype(jnp.bfloat16).astype(jnp.float32)
    return first, second, rest - second


def dot_nn(left, right, precision=None):
    return lax.dot_general(
        left, right, (((1,), (0,)), ((), ())), precision=precision, preferred_element_type=jnp.float32
    )


def dot_nt(left, right, precision=None):
    return lax.dot_general(
        left, right, (((1,), (1,)), ((), ())), precision=precision, preferred_element_type=jnp.float32
    )


SIDE = 16
BEGIN_FLOPS, PROJECT_FLOPS, STATE_FLOPS = 4 * 10**9, 2 * 10**9, 4 * 10**9


def source_rows(lane, step, depth):
    me = lax.axis_index("tp")
    owner = (((me // 2) ^ step) * 2) + ((me % 2) ^ lane)
    return pl.ds(pl.multiple_of(owner * depth, depth), depth)


def begin_kernel(rate_ref, value_ref, gain_ref, rate_out, value_out, gain_out):
    place = lax.axis_index("sp")
    heads, width = rate_out.shape
    head_at = lax.broadcasted_iota(jnp.int32, (heads, width), 0)
    rates = jnp.zeros((heads, width), jnp.float32)
    for head in range(heads):
        rates = jnp.where(head_at == head, rate_ref[head], rates)
    rate_out[...] = rates
    columns = gain_ref.shape[1]

    def placed(rows):
        padded = jnp.concatenate(
            [rows, jnp.zeros((rows.shape[0], width - columns), jnp.float32)], axis=1
        )
        return pltpu.roll(padded, place * columns, 1)

    for s in range(value_ref.shape[0]):
        value_out[s] = placed(value_ref[s].astype(jnp.float32))
    gain_out[...] = placed(gain_ref[...])


def partial_kernel(sources, s, *refs):
    pieces, (key_ref, value_ref, gate_ref) = refs[: len(sources)], refs[len(sources) : -2]
    total_ref, gates_ref = refs[-2:]
    positions = total_ref.shape[0]
    width = key_ref.shape[1]
    total_key = total_value = total_gate = 0.0
    for piece, (lane, step) in zip(pieces, sources):
        rows = source_rows(lane, step, piece.shape[1])
        block = piece[...] if step else piece[pl.ds(s * positions, positions), :]
        total_key += dot_nn(block, key_ref[rows, :])
        total_value += dot_nn(block, value_ref[rows, :])
        total_gate += dot_nt(gate_ref[:, rows], block)
    total_ref[:, :width] = total_key
    total_ref[:, width:] = total_value
    gates_ref[...] = total_gate


def project_kernel(sources, s, group, *refs):
    count = len(sources)
    pieces = refs[:count]
    total_ref, gates_ref, key_ref, value_ref, gate_ref = refs[count : count + 5]
    extra_ref, rate_ref, fresh_ref, gain_ref = refs[count + 5 : count + 9]
    outs = refs[count + 9 : count + 9 + group]
    key_sum, value_sum, gate_rows, decay_rows, strength_rows = refs[count + 9 + group :]
    place = lax.axis_index("sp")
    first_head = lax.axis_index("tp") * rate_ref.shape[0]
    heads, positions = extra_ref.shape[1:]
    wide = key_ref.shape[1]
    width = wide // heads
    share = heads // group
    total_key, total_value = total_ref[:, :wide], total_ref[:, wide:]
    total_gate = gates_ref[...]
    for piece, (lane, step) in zip(pieces, sources):
        rows = source_rows(lane, step, piece.shape[1])
        block = piece[...]
        total_key += dot_nn(block, key_ref[rows, :])
        total_value += dot_nn(block, value_ref[rows, :])
        total_gate += dot_nt(gate_ref[:, rows], block)
    gate_rows[...] = total_gate
    half = gate_rows.shape[0] // 2
    gates = [
        jnp.concatenate(
            [gate_rows[pl.ds(start + first_head + head, 1), :] for head in range(heads)], axis=0
        )
        for start in (0, half)
    ]
    key_sum[...] = total_key.astype(jnp.bfloat16)
    value_sum[...] = total_value.astype(jnp.bfloat16)
    row_at = lax.broadcasted_iota(jnp.int32, (positions, positions), 0)
    col_at = lax.broadcasted_iota(jnp.int32, (positions, positions), 1)
    upper = (row_at <= col_at).astype(jnp.bfloat16)
    decay = -rate_ref[...] * jax.nn.softplus(gates[0]) + extra_ref[s]
    parts = jnp.concatenate(split3(decay), axis=0).astype(jnp.bfloat16)
    summed = dot_nn(parts, upper)
    decay_rows[...] = summed[:heads] + summed[heads : 2 * heads] + summed[2 * heads :]
    strength_rows[...] = jax.nn.sigmoid(gates[1] - strength_offset)
    gain_parts = split3(gain_ref[...])
    for m in range(group):
        peer = place ^ m
        for r in range(share):
            head = peer * share + r
            columns = pl.ds(pl.multiple_of(head * width, width), width)
            outs[m][r, pl.ds(0, positions), :] = key_sum[:, columns]
            outs[m][r, pl.ds(positions, positions), :] = value_sum[:, columns]
            side = [
                *split3(decay_rows[pl.ds(head, 1), :]),
                *split3(strength_rows[pl.ds(head, 1), :]),
                fresh_ref[s, pl.ds(head, 1), :],
                *gain_parts,
            ]
            side.append(jnp.zeros((SIDE - len(side), positions), jnp.float32))
            outs[m][r, pl.ds(2 * positions, SIDE), :] = jnp.concatenate(side, axis=0).astype(
                jnp.bfloat16
            )


def halves(value):
    high = value.astype(jnp.bfloat16)
    return high, (value - high.astype(jnp.float32)).astype(jnp.bfloat16)


def dot_wide(left, right):
    left_high, left_low = halves(left)
    right_high, right_low = halves(right)
    columns = right.shape[1]
    both = dot_nn(
        jnp.concatenate([left_high, left_low], axis=1),
        jnp.concatenate(
            [
                jnp.concatenate([right_high, right_low], axis=1),
                jnp.concatenate([right_high, jnp.zeros_like(right_low)], axis=1),
            ],
            axis=0,
        ),
    )
    return both[:, :columns] + both[:, columns:]


def dot_left(left, right):
    return dot_nn(jnp.concatenate(halves(left), axis=1), jnp.concatenate([right, right], axis=0))


def over_unit_lower(lefts, mixings, row_at, col_at):
    extent = mixings[0].shape[0]
    small = 16

    def stacked(tops, bottoms, rights):
        pairs = [
            dot_wide(jnp.concatenate([top, bottom], axis=0), right)
            for top, bottom, right in zip(tops, bottoms, rights)
        ]
        return [pair[:extent] for pair in pairs], [pair[extent:] for pair in pairs]

    def powers(results, steps, covered, reach):
        while 2 * covered < reach:
            gains, squares = stacked(results, steps, steps)
            results = [result + gain for result, gain in zip(results, gains)]
            steps, covered = squares, 2 * covered
        return [result + dot_wide(result, step) for result, step in zip(results, steps)]

    inside = row_at // small == col_at // small
    steps = [jnp.where(inside, -mixing, 0.0) for mixing in mixings]
    eye = (row_at == col_at).astype(jnp.float32)
    diagonals = [eye + step for step in steps]
    diagonals = powers(diagonals, [dot_wide(step, step) for step in steps], 2, small)
    outside = [jnp.where(inside, 0.0, -mixing) for mixing in mixings]
    lefts, steps = stacked(lefts, outside, diagonals)
    return powers(lefts, steps, 1, extent // small)


def state_kernel(s, group, *refs):
    blocks = refs[:group]
    query_ref, new_key_ref, strengths = refs[group : group + 3]
    earlier = refs[group + 3 : -group - 3]
    outs = refs[-group - 3 : -3]
    maps, adds, turned = refs[-3:]
    for m in range(group if earlier else 0):
        outs[m][:s] = earlier[m][...]
    place = lax.axis_index("sp")
    share = blocks[0].shape[0]
    positions = (blocks[0].shape[1] - SIDE) // 2
    width = blocks[0].shape[2]
    row_at = lax.broadcasted_iota(jnp.int32, (positions, positions), 0)
    col_at = lax.broadcasted_iota(jnp.int32, (positions, positions), 1)
    eye = row_at == col_at
    units = [(r, m) for r in range(share) for m in range(group)]
    count = len(units)
    keys = [blocks[m][r, pl.ds(0, positions), :] for r, m in units]
    grams = [dot_nt(key, key) for key in keys]
    values = [blocks[m][r, pl.ds(positions, positions), :] for r, m in units]
    sides = [blocks[m][r, pl.ds(2 * positions, SIDE), :].astype(jnp.float32) for r, m in units]
    decays = [side[0:1] + side[1:2] + side[2:3] for side in sides]
    strength_rows = [side[3:4] + side[4:5] + side[5:6] for side in sides]
    lines = jnp.concatenate([*decays, jnp.zeros((-count % 8, positions), jnp.float32)], axis=0)
    columns = lines.T
    withins = [
        jnp.where(
            row_at > col_at,
            jnp.exp(jnp.where(row_at > col_at, columns[:, u : u + 1] - decays[u], 0.0)),
            0.0,
        )
        for u in range(count)
    ]
    turned_keys = [key.T.astype(jnp.float32) for key in keys]
    squares = [jnp.sum(jnp.where(eye, gram, 0.0), axis=0, keepdims=True) + 1e-06 for gram in grams]
    scales = [lax.rsqrt(square) for square in squares]
    mixings = [
        grams[u] * withins[u] * (strength_rows[u] * scales[u] * scales[u]) for u in range(count)
    ]
    finals = [row[:, positions - 1 :] for row in decays]
    lefts = [
        turned_keys[u] * (strength_rows[u] * scales[u] * scales[u] * jnp.exp(finals[u] - decays[u]))
        for u in range(count)
    ]
    lefts = over_unit_lower(lefts, mixings, row_at, col_at)
    for u, (r, m) in enumerate(units):
        slot = r * group + (place ^ m)
        adds[slot] = dot_left(lefts[u] * (squares[u] * scales[u]), values[u])
        erase = dot_left(lefts[u] * jnp.exp(decays[u]), keys[u])
        maps[slot] = jnp.where(eye, jnp.exp(finals[u]), 0.0) - erase
    for r in range(share):
        level = [(maps[r * group + b], adds[r * group + b]) for b in range(group)]
        while len(level) > 1:
            joined = []
            for b in range(0, len(level), 2):
                (first_map, first_add), (second_map, second_add) = level[b : b + 2]
                if b == 0:
                    joined.append((None, dot_wide(second_map, first_add) + second_add))
                else:
                    both = dot_wide(second_map, jnp.concatenate([first_map, first_add], axis=1))
                    joined.append((both[:, :width], both[:, width:] + second_add))
            level = joined
        state = level[0][1]
        head = place * share + r
        spot = pl.ds(pl.multiple_of(head * width, width), width)
        query = query_ref[:, spot].astype(jnp.float32)[s : s + 1]
        new_key = new_key_ref[:, spot].astype(jnp.float32)[s : s + 1]
        unit_new = new_key * lax.rsqrt(jnp.sum(new_key * new_key, axis=-1, keepdims=True) + 1e-06)
        both = jnp.concatenate([query, unit_new, jnp.zeros((6, width), jnp.float32)], axis=0)
        overlap = jnp.sum(query * unit_new, axis=-1, keepdims=True)
        lane_at = lax.broadcasted_iota(jnp.int32, strengths.shape, 1)
        strength = jnp.sum(jnp.where(lane_at == head, strengths[...], 0.0), axis=1, keepdims=True)
        fresh_row = sum(sides[r * group + m][6:7] for m in range(group))
        gain_row = sum(sides[r * group + m][j : j + 1] for m in range(group) for j in (7, 8, 9))
        reads = dot_wide(both, state)
        raw = reads[0:1] + strength[s : s + 1] * overlap * (fresh_row - reads[1:2])
        first = raw * lax.rsqrt(jnp.mean(raw * raw, axis=-1, keepdims=True) + 1e-06) * gain_row
        turned[...] = state.T.astype(jnp.bfloat16)
        tail = jnp.broadcast_to(first, (SIDE, first.shape[1])).astype(jnp.bfloat16)
        column_share = turned.shape[0] // group
        for m in range(group):
            rows = pl.ds(pl.multiple_of((place ^ m) * column_share, column_share), column_share)
            outs[m][s, r, pl.ds(0, column_share), :] = turned[rows, :]
            outs[m][s, r, pl.ds(column_share, SIDE), :] = tail


def finish_kernel(group, *refs):
    state_ref, read_ref, reads = refs[-3:]
    place = lax.axis_index("sp")
    sequences, share, rows, _ = refs[0].shape
    column_share = rows - SIDE
    for m in range(group):
        part = refs[m]
        for s in range(sequences):
            for r in range(share):
                head = (place ^ m) * share + r
                state_ref[s, head] = part[s, r, pl.ds(0, column_share), :]
                line = pltpu.roll(
                    part[s, r, pl.ds(column_share, SIDE), :].astype(jnp.float32)[:8],
                    (group - place) * column_share,
                    1,
                )
                reads[s, pl.ds(head, 1), :] = line[0:1, :column_share]
    read_ref[...] = reads[...].astype(jnp.bfloat16)


def fast_local(
    tokens,
    key_matrix,
    value_matrix,
    gate_matrix,
    head_decay_rate,
    extra_log_decay,
    next_token_query,
    next_token_key,
    next_token_value,
    next_write_strength,
    read_norm_gain,
):
    sequences, positions, depth = tokens.shape
    heads = head_decay_rate.shape[0]
    group = lax.axis_size("sp")
    members = lax.axis_size("tp")
    share = heads // group
    width = key_matrix.shape[1] // heads
    column_share = next_token_value.shape[2]
    value_width = column_share * group
    f32, bf16 = jnp.float32, jnp.bfloat16

    def over_tp(array, step):
        links = [(z * 2 + c, (z ^ step) * 2 + c) for z in range(members // 2) for c in range(2)]
        return lax.ppermute(array, "tp", links)

    def to_partner(array):
        return lax.ppermute(array, "tp", [(i, i ^ 1) for i in range(members)])

    def over_sp(array, step):
        return lax.ppermute(array, "sp", [(i, i ^ step) for i in range(group)])

    def after_all(array, *others):
        return lax.optimization_barrier((array, others))[0]

    def kernel(body, mib, flops, shapes, scratch, operands, specs=None):
        return pl.pallas_call(
            body,
            out_shape=[jax.ShapeDtypeStruct(*shape) for shape in shapes],
            in_specs=specs or [vmem] * len(operands),
            out_specs=[vmem] * len(shapes),
            scratch_shapes=scratch,
            compiler_params=pltpu.CompilerParams(vmem_limit_bytes=mib * 2**20),
            cost_estimate=pl.CostEstimate(flops=flops, bytes_accessed=0, transcendentals=0),
        )(*operands)

    vmem = pl.BlockSpec(memory_space=pltpu.VMEM)
    own = tokens.reshape(sequences * positions, depth)
    rows, out_rows = 2 * positions + SIDE, column_share + SIDE
    steps = range(1, members // 2)
    pairs = [(lane, step) for step in steps for lane in (0, 1)]
    got = [[over_tp(tokens[s], step) for step in steps] for s in range(sequences)]
    wide = key_matrix.shape[1]
    partner = to_partner(own)
    begun = kernel(
        begin_kernel,
        4,
        BEGIN_FLOPS,
        [
            ((heads, positions), f32),
            ((sequences, heads, value_width), f32),
            ((1, value_width), f32),
        ],
        [],
        [head_decay_rate, next_token_value, read_norm_gain[None]],
        [pl.BlockSpec(memory_space=pltpu.SMEM), vmem, vmem],
    )
    blocks, after = [], tuple(begun)
    for s in range(sequences):
        arrived = []
        for step, piece in zip(steps, got[s]):
            piece = after_all(piece, *(begun if step == steps[0] else after))
            arrived += [piece, to_partner(piece)]
        early = len(arrived) - 4
        weights = [key_matrix, value_matrix, gate_matrix.T]
        totals = kernel(
            functools.partial(partial_kernel, [(0, 0), (1, 0), *pairs[:early]], s),
            12,
            PROJECT_FLOPS,
            [((positions, 2 * wide), f32), ((gate_matrix.shape[1], positions), f32)],
            [],
            [own, partner, *arrived[:early], *weights],
        )
        messages = kernel(
            functools.partial(project_kernel, pairs[early:], s, group),
            12,
            PROJECT_FLOPS,
            [((share, rows, width), bf16)] * group,
            [
                pltpu.VMEM((positions, wide), bf16),
                pltpu.VMEM((positions, wide), bf16),
                pltpu.VMEM((gate_matrix.shape[1], positions), f32),
                pltpu.VMEM((heads, positions), f32),
                pltpu.VMEM((heads, positions), f32),
            ],
            [
                *arrived[early:],
                *totals,
                *weights,
                extra_log_decay,
                *begun,
            ],
        )
        after = tuple(messages)
        blocks.append([messages[0]] + [over_sp(messages[m], m) for m in range(1, group)])
    results = []
    for s in range(sequences):
        results = kernel(
            functools.partial(state_kernel, s, group),
            8,
            STATE_FLOPS,
            [((s + 1, share, out_rows, width), bf16)] * group,
            [
                pltpu.VMEM((heads, width, value_width), f32),
                pltpu.VMEM((heads, width, width), f32),
                pltpu.VMEM((value_width, width), bf16),
            ],
            [*blocks[s], next_token_query, next_token_key, next_write_strength, *results],
        )
    parts = [results[0]] + [over_sp(results[m], m) for m in range(1, group)]
    turned_state, first_read = kernel(
        functools.partial(finish_kernel, group),
        4,
        10**6,
        [((sequences, heads, column_share, width), bf16), ((sequences, heads, column_share), bf16)],
        [pltpu.VMEM((sequences, heads, column_share), f32)],
        parts,
    )
    return turned_state.transpose(0, 1, 3, 2), first_read


def pick(mesh):
    def body(*args):
        group, members = mesh.shape["sp"], mesh.shape["tp"]
        tokens, heads = args[0], args[4].shape[0]
        powers = group & (group - 1) == 0 and members & (members - 1) == 0
        square = args[1].shape[1] // heads == tokens.shape[1] == args[2].shape[1] // heads
        if powers and members > 1 and heads % group == 0 and square:
            return fast_local(*args)
        return local(*args)

    return body


def solution(mesh):
    in_specs = (
        P(None, "sp", "tp"),
        P(None, "tp"),
        P(None, "tp"),
        P(),
        P("tp"),
        P(None, "tp", "sp"),
        P(None, "tp"),
        P(None, "tp"),
        P(None, "tp", "sp"),
        P(None, "tp"),
        P("sp"),
    )
    out_specs = (P(None, "tp", None, "sp"), P(None, "tp", "sp"))
    return jax.shard_map(
        pick(mesh), mesh=mesh, in_specs=in_specs, out_specs=out_specs, check_vma=False)
```

```python
import functools

import jax
import jax.numpy as jnp
from jax import lax
from jax.experimental import pallas as pl
from jax.experimental.pallas import tpu as pltpu
from jax.sharding import PartitionSpec as P

DV = 128


exact_mode = lax.Precision.HIGHEST
strength_offset = 5.0


def unit_rows(matrix):
    return matrix * lax.rsqrt(jnp.sum(matrix * matrix, axis=-1, keepdims=True) + 1e-06)


def nilpotent_inverse(mixing):
    extent = mixing.shape[-1]
    result = jnp.zeros_like(mixing) + jnp.eye(extent, dtype=jnp.float32)
    powered = -mixing
    covered = 1
    while covered < extent:
        product = lax.optimization_barrier(
            jnp.einsum("...ij,...jk->...ik", result, powered, precision=exact_mode)
        )
        result = result + product
        powered = jnp.einsum("...ij,...jk->...ik", powered, powered, precision=exact_mode)
        covered = covered * 2
    return result


def block_terms(unit_keys, values, decay_logarithm, strength):
    extent = unit_keys.shape[-2]
    lower = jnp.tril(jnp.ones((extent, extent), jnp.bool_))
    strict = jnp.tril(jnp.ones((extent, extent), jnp.bool_), -1)
    running = jnp.cumsum(decay_logarithm, axis=-1)
    spread = running[..., :, None] - running[..., None, :]
    within = jnp.where(lower, jnp.exp(jnp.where(lower, spread, 0.0)), 0.0)
    scaled = unit_keys * strength[..., None]
    mixing = jnp.where(
        strict,
        jnp.einsum("...id,...jd->...ij", scaled, unit_keys, precision=exact_mode) * within,
        0.0,
    )
    inverse = nilpotent_inverse(mixing)
    writes = jnp.einsum(
        "...ij,...je->...ie", inverse, values * strength[..., None], precision=exact_mode
    )
    erases = jnp.einsum(
        "...ij,...jd->...id", inverse, scaled * jnp.exp(running)[..., None], precision=exact_mode
    )
    final_log = running[..., -1]
    carried = unit_keys * jnp.exp(final_log[..., None] - running)[..., None]
    return (writes, erases, carried, final_log)


def split_blocks(array, block_count):
    shaped = array.reshape(
        array.shape[:2] + (block_count, array.shape[2] // block_count) + array.shape[3:]
    )
    return jnp.moveaxis(shaped, 2, 0)


def local(
    tokens,
    key_matrix,
    value_matrix,
    gate_matrix,
    head_decay_rate,
    extra_log_decay,
    next_token_query,
    next_token_key,
    next_token_value,
    next_write_strength,
    read_norm_gain,
):
    sequences, positions, _ = tokens.shape
    local_heads = head_decay_rate.shape[0]
    key_width = key_matrix.shape[1] // local_heads
    value_width = value_matrix.shape[1] // local_heads
    all_heads = gate_matrix.shape[1] // 2
    group_size = lax.axis_size("sp")
    column_share = value_width // group_size
    first_head = lax.axis_index("tp") * local_heads
    decay_cols = lax.dynamic_slice_in_dim(gate_matrix, first_head, local_heads, 1)
    strength_cols = lax.dynamic_slice_in_dim(gate_matrix, all_heads + first_head, local_heads, 1)
    gate_cols = jnp.concatenate([decay_cols, strength_cols], axis=1)
    row_count = sequences * positions
    incoming = lax.all_gather(tokens, "tp", axis=2, tiled=True)
    span_width = incoming.shape[2]
    flat_rows = incoming.reshape(row_count, span_width)
    products = lax.optimization_barrier(
        (
            jnp.dot(flat_rows, key_matrix, preferred_element_type=jnp.float32),
            jnp.dot(flat_rows, value_matrix, preferred_element_type=jnp.float32),
            jnp.dot(flat_rows, gate_cols, preferred_element_type=jnp.float32),
        )
    )
    key_sum = products[0]
    value_sum = products[1]
    gate_pre = products[2]
    key_float = lax.optimization_barrier(key_sum.astype(jnp.bfloat16)).astype(jnp.float32)
    value_float = lax.optimization_barrier(value_sum.astype(jnp.bfloat16)).astype(jnp.float32)
    unit_keys = unit_rows(
        key_float.reshape(sequences, positions, local_heads, key_width).transpose(0, 2, 1, 3)
    )
    values = value_float.reshape(sequences, positions, local_heads, value_width).transpose(
        0, 2, 1, 3
    )
    gate_projected = gate_pre.reshape(sequences, positions, 2 * local_heads).transpose(0, 2, 1)
    decay_logarithm = (
        -head_decay_rate[None, :, None] * jax.nn.softplus(gate_projected[:, :local_heads])
        + extra_log_decay
    )
    strength = jax.nn.sigmoid(gate_projected[:, local_heads:] - strength_offset)
    block_count = positions // min(64, positions)
    block_parts = block_terms(
        split_blocks(unit_keys, block_count),
        split_blocks(values, block_count),
        split_blocks(decay_logarithm, block_count),
        split_blocks(strength, block_count),
    )
    identity = jnp.zeros((sequences, local_heads, key_width, key_width), jnp.float32) + jnp.eye(
        key_width, dtype=jnp.float32
    )
    start_map = jnp.concatenate(
        [identity, jnp.zeros((sequences, local_heads, key_width, value_width), jnp.float32)],
        axis=-1,
    )

    def advance(current, block_part):
        writes, erases, carried, final_log = block_part
        padded = jnp.concatenate(
            [jnp.zeros(writes.shape[:-1] + (key_width,), jnp.float32), writes], axis=-1
        )
        removed = lax.optimization_barrier(
            jnp.einsum("shcd,shde->shce", erases, current, precision=exact_mode)
        )
        fresh = padded - removed
        added = lax.optimization_barrier(
            jnp.einsum("shcd,shce->shde", carried, fresh, precision=exact_mode)
        )
        current = current * jnp.exp(final_log)[..., None, None] + added
        return (current, None)

    local_map, _ = lax.scan(advance, start_map, block_parts)
    carry_map = local_map[..., :key_width]
    write_map = local_map[..., key_width:]
    carry_copies = jnp.broadcast_to(carry_map[None], (group_size,) + carry_map.shape)
    write_parts = jnp.moveaxis(
        write_map.reshape(sequences, local_heads, key_width, group_size, column_share), 3, 0
    )
    carries = lax.all_to_all(carry_copies, "sp", split_axis=0, concat_axis=0, tiled=True)
    write_cols = lax.all_to_all(write_parts, "sp", split_axis=0, concat_axis=0, tiled=True)

    def fold_step(current, block_map):
        moved = lax.optimization_barrier(
            jnp.einsum("shij,shje->shie", block_map[0], current, precision=exact_mode)
        )
        return (moved + block_map[1], None)

    begin_state = jnp.zeros(write_cols.shape[1:], jnp.float32)
    folded, _ = lax.scan(fold_step, begin_state, (carries, write_cols))
    query_rows = next_token_query.astype(jnp.float32).reshape(sequences, local_heads, key_width)
    unit_new = unit_rows(
        next_token_key.astype(jnp.float32).reshape(sequences, local_heads, key_width)
    )
    value_rows = next_token_value.astype(jnp.float32)
    key_read = jnp.einsum("shd,shde->she", unit_new, folded, precision=exact_mode)
    query_read = jnp.einsum("shd,shde->she", query_rows, folded, precision=exact_mode)
    intersection = jnp.sum(query_rows * unit_new, axis=-1)
    read_raw = query_read + (next_write_strength * intersection)[..., None] * (
        value_rows - key_read
    )
    square_total = lax.psum(jnp.sum(read_raw * read_raw, axis=-1, keepdims=True), "sp")
    first_read = read_raw * lax.rsqrt(square_total / DV + 1e-06) * read_norm_gain
    return (folded.astype(jnp.bfloat16), first_read.astype(jnp.bfloat16))


def split3(value):
    first = value.astype(jnp.bfloat16).astype(jnp.float32)
    rest = value - first
    second = rest.astype(jnp.bfloat16).astype(jnp.float32)
    return first, second, rest - second


def dot_nn(left, right, precision=None):
    return lax.dot_general(
        left, right, (((1,), (0,)), ((), ())), precision=precision, preferred_element_type=jnp.float32
    )


def dot_nt(left, right, precision=None):
    return lax.dot_general(
        left, right, (((1,), (1,)), ((), ())), precision=precision, preferred_element_type=jnp.float32
    )


SIDE = 16
BEGIN_FLOPS, PROJECT_FLOPS, STATE_FLOPS = 4 * 10**9, 2 * 10**9, 4 * 10**9


def source_rows(lane, step, depth):
    me = lax.axis_index("tp")
    owner = (((me // 2) ^ step) * 2) + ((me % 2) ^ lane)
    return pl.ds(pl.multiple_of(owner * depth, depth), depth)


def begin_kernel(rate_ref, value_ref, gain_ref, rate_out, value_out, gain_out):
    place = lax.axis_index("sp")
    heads, width = rate_out.shape
    head_at = lax.broadcasted_iota(jnp.int32, (heads, width), 0)
    rates = jnp.zeros((heads, width), jnp.float32)
    for head in range(heads):
        rates = jnp.where(head_at == head, rate_ref[head], rates)
    rate_out[...] = rates
    columns = gain_ref.shape[1]

    def placed(rows):
        padded = jnp.concatenate(
            [rows, jnp.zeros((rows.shape[0], width - columns), jnp.float32)], axis=1
        )
        return pltpu.roll(padded, place * columns, 1)

    for s in range(value_ref.shape[0]):
        value_out[s] = placed(value_ref[s].astype(jnp.float32))
    gain_out[...] = placed(gain_ref[...])


def partial_kernel(sources, s, chained, *refs):
    before, refs = (refs[:2], refs[2:]) if chained else ((), refs)
    pieces, (key_ref, value_ref, gate_ref) = refs[: len(sources)], refs[len(sources) : -2]
    total_ref, gates_ref = refs[-2:]
    positions = total_ref.shape[0]
    width = key_ref.shape[1]
    total_key = total_value = total_gate = 0.0
    if chained:
        total_key, total_value = before[0][:, :width], before[0][:, width:]
        total_gate = before[1][...]
    for piece, (lane, step) in zip(pieces, sources):
        rows = source_rows(lane, step, piece.shape[1])
        block = piece[...] if step else piece[pl.ds(s * positions, positions), :]
        total_key += dot_nn(block, key_ref[rows, :])
        total_value += dot_nn(block, value_ref[rows, :])
        total_gate += dot_nt(gate_ref[:, rows], block)
    total_ref[:, :width] = total_key
    total_ref[:, width:] = total_value
    gates_ref[...] = total_gate


def project_kernel(sources, s, group, *refs):
    count = len(sources)
    pieces = refs[:count]
    total_ref, gates_ref, key_ref, value_ref, gate_ref = refs[count : count + 5]
    extra_ref, rate_ref, fresh_ref, gain_ref = refs[count + 5 : count + 9]
    outs = refs[count + 9 : count + 9 + group]
    key_sum, value_sum, gate_rows, decay_rows, strength_rows = refs[count + 9 + group :]
    place = lax.axis_index("sp")
    first_head = lax.axis_index("tp") * rate_ref.shape[0]
    heads, positions = extra_ref.shape[1:]
    wide = key_ref.shape[1]
    width = wide // heads
    share = heads // group
    total_key, total_value = total_ref[:, :wide], total_ref[:, wide:]
    total_gate = gates_ref[...]
    for piece, (lane, step) in zip(pieces, sources):
        rows = source_rows(lane, step, piece.shape[1])
        block = piece[...]
        total_key += dot_nn(block, key_ref[rows, :])
        total_value += dot_nn(block, value_ref[rows, :])
        total_gate += dot_nt(gate_ref[:, rows], block)
    gate_rows[...] = total_gate
    half = gate_rows.shape[0] // 2
    gates = [
        jnp.concatenate(
            [gate_rows[pl.ds(start + first_head + head, 1), :] for head in range(heads)], axis=0
        )
        for start in (0, half)
    ]
    key_sum[...] = total_key.astype(jnp.bfloat16)
    value_sum[...] = total_value.astype(jnp.bfloat16)
    row_at = lax.broadcasted_iota(jnp.int32, (positions, positions), 0)
    col_at = lax.broadcasted_iota(jnp.int32, (positions, positions), 1)
    upper = (row_at <= col_at).astype(jnp.bfloat16)
    decay = -rate_ref[...] * jax.nn.softplus(gates[0]) + extra_ref[s]
    parts = jnp.concatenate(split3(decay), axis=0).astype(jnp.bfloat16)
    summed = dot_nn(parts, upper)
    decay_rows[...] = summed[:heads] + summed[heads : 2 * heads] + summed[2 * heads :]
    strength_rows[...] = jax.nn.sigmoid(gates[1] - strength_offset)
    gain_parts = split3(gain_ref[...])
    for m in range(group):
        peer = place ^ m
        for r in range(share):
            head = peer * share + r
            columns = pl.ds(pl.multiple_of(head * width, width), width)
            outs[m][r, pl.ds(0, positions), :] = key_sum[:, columns]
            outs[m][r, pl.ds(positions, positions), :] = value_sum[:, columns]
            side = [
                *split3(decay_rows[pl.ds(head, 1), :]),
                *split3(strength_rows[pl.ds(head, 1), :]),
                fresh_ref[s, pl.ds(head, 1), :],
                *gain_parts,
            ]
            side.append(jnp.zeros((SIDE - len(side), positions), jnp.float32))
            outs[m][r, pl.ds(2 * positions, SIDE), :] = jnp.concatenate(side, axis=0).astype(
                jnp.bfloat16
            )


def halves(value):
    high = value.astype(jnp.bfloat16)
    return high, (value - high.astype(jnp.float32)).astype(jnp.bfloat16)


def dot_wide(left, right):
    left_high, left_low = halves(left)
    right_high, right_low = halves(right)
    columns = right.shape[1]
    both = dot_nn(
        jnp.concatenate([left_high, left_low], axis=1),
        jnp.concatenate(
            [
                jnp.concatenate([right_high, right_low], axis=1),
                jnp.concatenate([right_high, jnp.zeros_like(right_low)], axis=1),
            ],
            axis=0,
        ),
    )
    return both[:, :columns] + both[:, columns:]


def dot_left(left, right):
    return dot_nn(jnp.concatenate(halves(left), axis=1), jnp.concatenate([right, right], axis=0))


def over_unit_lower(lefts, mixings, row_at, col_at):
    extent = mixings[0].shape[0]
    small = 16

    def stacked(tops, bottoms, rights):
        pairs = [
            dot_wide(jnp.concatenate([top, bottom], axis=0), right)
            for top, bottom, right in zip(tops, bottoms, rights)
        ]
        return [pair[:extent] for pair in pairs], [pair[extent:] for pair in pairs]

    def powers(results, steps, covered, reach):
        while 2 * covered < reach:
            gains, squares = stacked(results, steps, steps)
            results = [result + gain for result, gain in zip(results, gains)]
            steps, covered = squares, 2 * covered
        return [result + dot_wide(result, step) for result, step in zip(results, steps)]

    inside = row_at // small == col_at // small
    steps = [jnp.where(inside, -mixing, 0.0) for mixing in mixings]
    eye = (row_at == col_at).astype(jnp.float32)
    diagonals = [eye + step for step in steps]
    diagonals = powers(diagonals, [dot_wide(step, step) for step in steps], 2, small)
    outside = [jnp.where(inside, 0.0, -mixing) for mixing in mixings]
    lefts, steps = stacked(lefts, outside, diagonals)
    return powers(lefts, steps, 1, extent // small)


def block_maps(keys, values, sides):
    count = len(keys)
    positions = keys[0].shape[0]
    row_at = lax.broadcasted_iota(jnp.int32, (positions, positions), 0)
    col_at = lax.broadcasted_iota(jnp.int32, (positions, positions), 1)
    eye = row_at == col_at
    grams = [dot_nt(key, key) for key in keys]
    decays = [side[0:1] + side[1:2] + side[2:3] for side in sides]
    strength_rows = [side[3:4] + side[4:5] + side[5:6] for side in sides]
    lines = jnp.concatenate([*decays, jnp.zeros((-count % 8, positions), jnp.float32)], axis=0)
    columns = lines.T
    withins = [
        jnp.where(
            row_at > col_at,
            jnp.exp(jnp.where(row_at > col_at, columns[:, u : u + 1] - decays[u], 0.0)),
            0.0,
        )
        for u in range(count)
    ]
    turned_keys = [key.T.astype(jnp.float32) for key in keys]
    squares = [jnp.sum(jnp.where(eye, gram, 0.0), axis=0, keepdims=True) + 1e-06 for gram in grams]
    scales = [lax.rsqrt(square) for square in squares]
    mixings = [
        grams[u] * withins[u] * (strength_rows[u] * scales[u] * scales[u]) for u in range(count)
    ]
    finals = [row[:, positions - 1 :] for row in decays]
    lefts = [
        turned_keys[u] * (strength_rows[u] * scales[u] * scales[u] * jnp.exp(finals[u] - decays[u]))
        for u in range(count)
    ]
    lefts = over_unit_lower(lefts, mixings, row_at, col_at)
    results = []
    for u in range(count):
        add = dot_left(lefts[u] * (squares[u] * scales[u]), values[u])
        erase = dot_left(lefts[u] * jnp.exp(decays[u]), keys[u])
        read_map = jnp.where(eye, jnp.exp(finals[u]), 0.0) - erase
        results.append(jnp.concatenate([read_map, add], axis=1))
    return results


def state_kernel(s, last, group, *refs):
    refs = list(refs)
    blocks = [refs.pop(0) for _ in range(group)]
    query_ref, new_key_ref, strengths = (refs.pop(0) for _ in range(3))
    earlier = [refs.pop(0) for _ in range(group)] if s else []
    held = refs.pop(0) if s else None
    following = None if last else refs.pop(0)
    outs = [refs.pop(0) for _ in range(group)]
    held_out = None if last else refs.pop(0)
    maps, turned = refs
    for before, out in zip(earlier, outs):
        out[:s] = before[...]
    place = lax.axis_index("sp")
    share = blocks[0].shape[0]
    positions = (blocks[0].shape[1] - SIDE) // 2
    width = blocks[0].shape[2]

    def taken(ref, r):
        return (
            ref[r, pl.ds(0, positions), :],
            ref[r, pl.ds(positions, positions), :],
            ref[r, pl.ds(2 * positions, SIDE), :].astype(jnp.float32),
        )

    units = [(r, m) for r in range(share) for m in range(group) if m or held is None]
    sources = [taken(blocks[m], r) for r, m in units]
    if following is not None:
        sources += [taken(following, r) for r in range(share)]
    results = block_maps(*zip(*sources))
    for (r, m), result in zip(units, results):
        maps[r * group + (place ^ m)] = result
    for r in range(share):
        if held is not None:
            maps[r * group + place] = held[r]
        if following is not None:
            held_out[r] = results[len(units) + r]
    for r in range(share):
        level = [
            (maps[r * group + b, :, :width], maps[r * group + b, :, width:]) for b in range(group)
        ]
        while len(level) > 1:
            joined = []
            for b in range(0, len(level), 2):
                (first_map, first_add), (second_map, second_add) = level[b : b + 2]
                if b == 0:
                    joined.append((None, dot_wide(second_map, first_add) + second_add))
                else:
                    both = dot_wide(second_map, jnp.concatenate([first_map, first_add], axis=1))
                    joined.append((both[:, :width], both[:, width:] + second_add))
            level = joined
        state = level[0][1]
        head = place * share + r
        spot = pl.ds(pl.multiple_of(head * width, width), width)
        query = query_ref[:, spot].astype(jnp.float32)[s : s + 1]
        new_key = new_key_ref[:, spot].astype(jnp.float32)[s : s + 1]
        unit_new = new_key * lax.rsqrt(jnp.sum(new_key * new_key, axis=-1, keepdims=True) + 1e-06)
        both = jnp.concatenate([query, unit_new, jnp.zeros((6, width), jnp.float32)], axis=0).T
        overlap = jnp.sum(query * unit_new, axis=-1, keepdims=True)
        lane_at = lax.broadcasted_iota(jnp.int32, strengths.shape, 1)
        strength = jnp.sum(jnp.where(lane_at == head, strengths[...], 0.0), axis=1, keepdims=True)
        sides = [
            block[r, pl.ds(2 * positions, SIDE), :].astype(jnp.float32) for block in blocks
        ]
        fresh_row = sum(side[6:7] for side in sides)
        gain_row = sum(side[j : j + 1] for side in sides for j in (7, 8, 9))
        query_read = jnp.sum(both[:, 0:1] * state, axis=0, keepdims=True)
        key_read = jnp.sum(both[:, 1:2] * state, axis=0, keepdims=True)
        raw = query_read + strength[s : s + 1] * overlap * (fresh_row - key_read)
        first = raw * lax.rsqrt(jnp.mean(raw * raw, axis=-1, keepdims=True) + 1e-06) * gain_row
        turned[...] = state.T.astype(jnp.bfloat16)
        tail = jnp.broadcast_to(first, (SIDE, first.shape[1])).astype(jnp.bfloat16)
        column_share = turned.shape[0] // group
        for m in range(group):
            rows = pl.ds(pl.multiple_of((place ^ m) * column_share, column_share), column_share)
            outs[m][s, r, pl.ds(0, column_share), :] = turned[rows, :]
            outs[m][s, r, pl.ds(column_share, SIDE), :] = tail


def finish_kernel(group, *refs):
    state_ref, read_ref, reads = refs[-3:]
    place = lax.axis_index("sp")
    sequences, share, rows, _ = refs[0].shape
    column_share = rows - SIDE
    for m in range(group):
        part = refs[m]
        for s in range(sequences):
            for r in range(share):
                head = (place ^ m) * share + r
                state_ref[s, head] = part[s, r, pl.ds(0, column_share), :]
                line = pltpu.roll(
                    part[s, r, pl.ds(column_share, SIDE), :].astype(jnp.float32)[:8],
                    (group - place) * column_share,
                    1,
                )
                reads[s, pl.ds(head, 1), :] = line[0:1, :column_share]
    read_ref[...] = reads[...].astype(jnp.bfloat16)


def fast_local(
    tokens,
    key_matrix,
    value_matrix,
    gate_matrix,
    head_decay_rate,
    extra_log_decay,
    next_token_query,
    next_token_key,
    next_token_value,
    next_write_strength,
    read_norm_gain,
):
    sequences, positions, depth = tokens.shape
    heads = head_decay_rate.shape[0]
    group = lax.axis_size("sp")
    members = lax.axis_size("tp")
    share = heads // group
    width = key_matrix.shape[1] // heads
    column_share = next_token_value.shape[2]
    value_width = column_share * group
    f32, bf16 = jnp.float32, jnp.bfloat16

    def over_tp(array, step):
        links = [(z * 2 + c, (z ^ step) * 2 + c) for z in range(members // 2) for c in range(2)]
        return lax.ppermute(array, "tp", links)

    def to_partner(array):
        return lax.ppermute(array, "tp", [(i, i ^ 1) for i in range(members)])

    def over_sp(array, step):
        return lax.ppermute(array, "sp", [(i, i ^ step) for i in range(group)])

    def after_all(array, *others):
        return lax.optimization_barrier((array, others))[0]

    def kernel(body, mib, flops, shapes, scratch, operands, specs=None):
        return pl.pallas_call(
            body,
            out_shape=[jax.ShapeDtypeStruct(*shape) for shape in shapes],
            in_specs=specs or [vmem] * len(operands),
            out_specs=[vmem] * len(shapes),
            scratch_shapes=scratch,
            compiler_params=pltpu.CompilerParams(vmem_limit_bytes=mib * 2**20),
            cost_estimate=pl.CostEstimate(flops=flops, bytes_accessed=0, transcendentals=0),
        )(*operands)

    vmem = pl.BlockSpec(memory_space=pltpu.VMEM)
    own = tokens.reshape(sequences * positions, depth)
    rows, out_rows = 2 * positions + SIDE, column_share + SIDE
    steps = range(1, members // 2)
    pairs = [(lane, step) for step in steps for lane in (0, 1)]
    got = [[over_tp(tokens[s], step) for step in steps] for s in range(sequences)]
    wide = key_matrix.shape[1]
    partner = to_partner(own)
    begun = kernel(
        begin_kernel,
        4,
        BEGIN_FLOPS,
        [
            ((heads, positions), f32),
            ((sequences, heads, value_width), f32),
            ((1, value_width), f32),
        ],
        [],
        [head_decay_rate, next_token_value, read_norm_gain[None]],
        [pl.BlockSpec(memory_space=pltpu.SMEM), vmem, vmem],
    )
    blocks, after = [], tuple(begun)
    for s in range(sequences):
        arrived = []
        for step, piece in zip(steps, got[s]):
            piece = after_all(piece, *(begun if step == steps[0] else after))
            arrived += [piece, to_partner(piece)]
        early = len(arrived) - 4
        weights = [key_matrix, value_matrix, gate_matrix.T]
        late = list(range(early, len(arrived)))
        stages = [([(0, 0), (1, 0), *pairs[:early]], [own, partner, *arrived[:early]])]
        if s:
            here, late = late[::2], late[1::2]
            stages.append(([pairs[n] for n in here], [arrived[n] for n in here]))
        totals = []
        for n, (sources, pieces) in enumerate(stages):
            totals = kernel(
                functools.partial(partial_kernel, sources, s, n > 0),
                12,
                PROJECT_FLOPS,
                [((positions, 2 * wide), f32), ((gate_matrix.shape[1], positions), f32)],
                [],
                [*totals, *pieces, *weights],
            )
        messages = kernel(
            functools.partial(project_kernel, [pairs[n] for n in late], s, group),
            12,
            PROJECT_FLOPS,
            [((share, rows, width), bf16)] * group,
            [
                pltpu.VMEM((positions, wide), bf16),
                pltpu.VMEM((positions, wide), bf16),
                pltpu.VMEM((gate_matrix.shape[1], positions), f32),
                pltpu.VMEM((heads, positions), f32),
                pltpu.VMEM((heads, positions), f32),
            ],
            [
                *(arrived[n] for n in late),
                *totals,
                *weights,
                extra_log_decay,
                *begun,
            ],
        )
        after = tuple(messages)
        blocks.append([messages[0]] + [over_sp(messages[m], m) for m in range(1, group)])
    results, held = [], []
    for s in range(sequences):
        last = s + 1 == sequences
        map_shape = ((share, width, width + value_width), f32)
        results = kernel(
            functools.partial(state_kernel, s, last, group),
            8,
            STATE_FLOPS,
            [((s + 1, share, out_rows, width), bf16)] * group + ([] if last else [map_shape]),
            [
                pltpu.VMEM((heads, width, width + value_width), f32),
                pltpu.VMEM((value_width, width), bf16),
            ],
            [
                *blocks[s],
                next_token_query,
                next_token_key,
                next_write_strength,
                *results,
                *held,
                *([] if last else [blocks[s + 1][0]]),
            ],
        )
        held, results = results[group:], results[:group]
    parts = [results[0]] + [over_sp(results[m], m) for m in range(1, group)]
    turned_state, first_read = kernel(
        functools.partial(finish_kernel, group),
        4,
        10**6,
        [((sequences, heads, column_share, width), bf16), ((sequences, heads, column_share), bf16)],
        [pltpu.VMEM((sequences, heads, column_share), f32)],
        parts,
    )
    return turned_state.transpose(0, 1, 3, 2), first_read


def pick(mesh):
    def body(*args):
        group, members = mesh.shape["sp"], mesh.shape["tp"]
        tokens, heads = args[0], args[4].shape[0]
        powers = group & (group - 1) == 0 and members & (members - 1) == 0
        square = args[1].shape[1] // heads == tokens.shape[1] == args[2].shape[1] // heads
        if powers and members > 1 and heads % group == 0 and square:
            return fast_local(*args)
        return local(*args)

    return body


def solution(mesh):
    in_specs = (
        P(None, "sp", "tp"),
        P(None, "tp"),
        P(None, "tp"),
        P(),
        P("tp"),
        P(None, "tp", "sp"),
        P(None, "tp"),
        P(None, "tp"),
        P(None, "tp", "sp"),
        P(None, "tp"),
        P("sp"),
    )
    out_specs = (P(None, "tp", None, "sp"), P(None, "tp", "sp"))
    return jax.shard_map(
        pick(mesh), mesh=mesh, in_specs=in_specs, out_specs=out_specs, check_vma=False)
```
